32 devices in a mesh: sp: 8 (over z, x), dp: 4 (over y, core).
Axes of the slice: x: 2, y: 2, z: 4, core: 2. Of those that a mesh axis runs over, the one named last changes fastest.
Arguments:
- inputs: bfloat16 [4, 2048, 2048], P('dp', 'sp'), may hold values from -6 to 6
- up_pre: bfloat16 [4, 2048, 1024], P('dp', 'sp'), may hold values from -6 to 6
- gate_pre: bfloat16 [4, 2048, 1024], P('dp', 'sp'), may hold values from -6 to 6
- cotangent: bfloat16 [4, 2048, 1024], P('dp', 'sp'), may hold values from -6 to 6
- norm_gain: float32 [1024], replicated, may hold values from 0.1 to 1.9
- up_weight: bfloat16 [2048, 1024], P('dp'), may hold values from -0.125 to 0.125
- gate_weight: bfloat16 [2048, 1024], P('dp'), may hold values from -0.125 to 0.125
- mix_weight: bfloat16 [8, 512, 512], replicated, may hold values from -0.375 to 0.375
Outputs:
- input_grad: bfloat16 [4, 2048, 2048], P('dp', 'sp')
- up_weight_grad: float32 [2048, 1024], P('dp')
- gate_weight_grad: float32 [2048, 1024], P('dp')
The draws below stay inside these ranges and needn't reach their ends.
All inputs are finite; a program needn't handle non-finite values.
Results may differ from the reference program's by a relative error of at most 0.0064.
Values may be sent and summed in bfloat16 or wider, within the bound.
No kernel may reach another device: no remote copies, remote signals or barrier semaphores. Data moves between devices by JAX's collectives and lax.ppermute only.
A program may use at most 128 MiB of HBM per device.

```python
import math
import jax
import jax.numpy as jnp
from jax import lax

MODEL = 2048
GROUPS = 8
GROUP_CH = 128
SPAN = 512
SEG = 64
GATED = 1024
LENGTH = 2048
BATCH = 4


def levels(stream_key, dims, pieces, smallest, high):
    loudness = 1.0
    for axis_at, parts in pieces:
        draws = jax.random.uniform(jax.random.fold_in(jax.random.fold_in(stream_key, 6), axis_at), (parts,), jnp.float32, smallest / len(pieces), high / len(pieces))
        loudness = loudness * jnp.repeat(jnp.exp(draws), dims[axis_at] // parts).reshape((-1,) + (1,) * (len(dims) - 1 - axis_at))
    return loudness


def noise(own_key, shape, deviation, reach, split=(), dtype=jnp.bfloat16):
    entries = deviation * jax.random.normal(own_key, shape, jnp.float32)
    if split:
        entries = entries * levels(own_key, shape, split, -0.22, 0.18)
    return jnp.clip(entries, -reach, reach).astype(dtype)


def setup_inputs(seed: int = 0) -> dict:
    key_list = jax.random.split(jax.random.key(seed), 9)
    inputs = noise(key_list[0], (BATCH, LENGTH, MODEL), 1.0, 6.0, ((0, 4), (1, 8)))
    up_pre = noise(key_list[1], (BATCH, LENGTH, GATED), 1.0, 6.0, ((0, 4), (1, 8)))
    gate_pre = noise(key_list[2], (BATCH, LENGTH, GATED), 1.0, 6.0, ((0, 4), (1, 8)))
    cotangent = noise(key_list[3], (BATCH, LENGTH, GATED), 1.0, 6.0, ((0, 4), (1, 8)))
    norm_gain = jnp.clip(1.0 + 0.18 * jax.random.normal(key_list[4], (GATED,), jnp.float32), 0.1, 1.9)
    up_weight = noise(key_list[5], (MODEL, GATED), MODEL ** -0.5, 0.125, ((0, 4),))
    gate_weight = noise(key_list[6], (MODEL, GATED), MODEL ** -0.5, 0.125, ((0, 4),))
    mix_weight = noise(key_list[7], (GROUPS, SPAN, SPAN), (SPAN // 2) ** -0.5, 0.375)
    return dict(inputs=inputs, up_pre=up_pre, gate_pre=gate_pre, cotangent=cotangent, norm_gain=norm_gain, up_weight=up_weight, gate_weight=gate_weight, mix_weight=mix_weight)


norm_eps = 1e-05
grad_scale = 1.0 / 256.0
root_half = 1.0 / math.sqrt(2.0)
root_twopi = 1.0 / math.sqrt(2.0 * math.pi)

def gelu_value(preact):
    return 0.5 * preact * (1.0 + lax.erf(preact * root_half))

def gelu_slope(preact):
    return 0.5 * (1.0 + lax.erf(preact * root_half)) + preact * jnp.exp(-0.5 * preact * preact) * root_twopi

def span_mask():
    segment = jnp.arange(SPAN) // SEG
    return segment[None, :] <= segment[:, None]

def reference(inputs, up_pre, gate_pre, cotangent, norm_gain, up_weight, gate_weight, mix_weight):
    up_float = up_pre.astype(jnp.float32)
    gate_float = gate_pre.astype(jnp.float32)
    grad_float = cotangent.astype(jnp.float32)
    gated_act = gelu_value(gate_float)
    centered = gated_act - lax.optimization_barrier(jnp.mean(gated_act, axis=-1, keepdims=True))
    inverse_std = lax.rsqrt(lax.optimization_barrier(jnp.mean(centered * centered, axis=-1, keepdims=True)) + norm_eps)
    normed = centered * inverse_std
    mixer_in = (normed * norm_gain).astype(jnp.bfloat16)
    mixer_grad = (grad_float * gelu_value(up_float)).astype(jnp.bfloat16)
    masked = jnp.where(span_mask()[None], mix_weight, jnp.zeros_like(mix_weight)).astype(jnp.float32)
    block_count = LENGTH // SPAN
    block_shape = (BATCH, block_count, SPAN, GROUPS, GROUP_CH)
    input_blocks = mixer_in.astype(jnp.float32).reshape(block_shape)
    grad_blocks = mixer_grad.astype(jnp.float32).reshape(block_shape)
    spatial = jnp.einsum('gts,bnsgc->bntgc', masked, input_blocks).astype(jnp.bfloat16)
    spatial = spatial.reshape(BATCH, LENGTH, GATED)
    normed_back = jnp.einsum('gts,bntgc->bnsgc', masked, grad_blocks).astype(jnp.bfloat16)
    normed_back = normed_back.reshape(BATCH, LENGTH, GATED)
    up_pre_grad = (grad_float * spatial.astype(jnp.float32) * gelu_slope(up_float)).astype(jnp.bfloat16)
    scaled = normed_back.astype(jnp.float32) * norm_gain
    gated_grad = inverse_std * (scaled - lax.optimization_barrier(jnp.mean(scaled, axis=-1, keepdims=True)) - normed * lax.optimization_barrier(jnp.mean(scaled * normed, axis=-1, keepdims=True)))
    gate_pre_grad = (gated_grad * gelu_slope(gate_float)).astype(jnp.bfloat16)
    flat_up = up_pre_grad.reshape(-1, GATED)
    flat_gate = gate_pre_grad.reshape(-1, GATED)
    flat_inputs = inputs.reshape(-1, MODEL)
    input_grad = jnp.dot(flat_up, up_weight.T, preferred_element_type=jnp.float32) + jnp.dot(flat_gate, gate_weight.T, preferred_element_type=jnp.float32)
    input_grad = input_grad.astype(jnp.bfloat16).reshape(BATCH, LENGTH, MODEL)
    up_weight_grad = jnp.dot(flat_inputs.T, flat_up, preferred_element_type=jnp.float32) * grad_scale
    gate_weight_grad = jnp.dot(flat_inputs.T, flat_gate, preferred_element_type=jnp.float32) * grad_scale
    return (input_grad, up_weight_grad, gate_weight_grad)
```

```python
import math

import jax
import jax.numpy as jnp
from jax import lax
from jax.experimental import pallas as pl
from jax.experimental.pallas import tpu as pltpu
from jax.sharding import PartitionSpec as P

GROUP_CH = 128
SPAN = 512
SEG = 64
ROW_STEP = 32

norm_eps = 1e-05
grad_scale = 1.0 / 256.0
root_half = 1.0 / math.sqrt(2.0)
root_twopi = 1.0 / math.sqrt(2.0 * math.pi)

WHOLE = pl.BlockSpec(memory_space=pltpu.VMEM)
SCALAR = pl.BlockSpec(memory_space=pltpu.SMEM)


def normal_cdf(preact):
    return 0.5 * (1.0 + lax.erf(preact * root_half))


def gelu_slope(preact, cdf):
    return cdf + preact * jnp.exp(-0.5 * preact * preact) * root_twopi


def norm_stats(gate):
    gated_act = gate * normal_cdf(gate)
    width = gate.shape[1]
    centered = gated_act - jnp.sum(gated_act, axis=-1, keepdims=True) * (1.0 / width)
    variance = jnp.sum(centered * centered, axis=-1, keepdims=True) * (1.0 / width)
    inverse_std = lax.rsqrt(variance + norm_eps)
    return centered * inverse_std, inverse_std


def row_loop(rows, body):
    def step(at, carry):
        body(pl.ds(pl.multiple_of(at * ROW_STEP, ROW_STEP), ROW_STEP))
        return carry

    lax.fori_loop(0, rows // ROW_STEP, step, 0)


def send_kernel(second_ref, up_ref, gate_ref, grad_ref, gain_ref, send_ref):
    rows = up_ref.shape[0]

    @pl.when(second_ref[0] == 0)
    def _():
        def body(at):
            normed, _ = norm_stats(gate_ref[at, :].astype(jnp.float32))
            send_ref[at, :] = (normed * gain_ref[...]).astype(jnp.bfloat16)

        row_loop(rows, body)

    @pl.when(second_ref[0] != 0)
    def _():
        def body(at):
            up = up_ref[at, :].astype(jnp.float32)
            mixed = grad_ref[at, :].astype(jnp.float32) * (up * normal_cdf(up))
            send_ref[at, :] = mixed.astype(jnp.bfloat16)

        row_loop(rows, body)


def own_kernel(
    up_ref, gate_ref, grad_ref, gain_ref, own_mix_ref,
    spatial_ref, back_ref, normed_ref, std_ref, up_slope_ref, gate_slope_ref,
    in_ref, mgrad_ref,
):
    rows, width = up_ref.shape

    def body(at):
        gate = gate_ref[at, :].astype(jnp.float32)
        normed, inverse_std = norm_stats(gate)
        normed_ref[at, :] = normed
        std_ref[at, :] = jnp.broadcast_to(inverse_std, (ROW_STEP, GROUP_CH))
        in_ref[at, :] = (normed * gain_ref[...]).astype(jnp.bfloat16)
        gate_slope_ref[at, :] = gelu_slope(gate, normal_cdf(gate))
        up = up_ref[at, :].astype(jnp.float32)
        grad = grad_ref[at, :].astype(jnp.float32)
        cdf = normal_cdf(up)
        mgrad_ref[at, :] = (grad * (up * cdf)).astype(jnp.bfloat16)
        up_slope_ref[at, :] = grad * gelu_slope(up, cdf)

    row_loop(rows, body)
    row_seg = lax.broadcasted_iota(jnp.int32, (rows, rows), 0) // SEG
    col_seg = lax.broadcasted_iota(jnp.int32, (rows, rows), 1) // SEG
    keep = col_seg <= row_seg
    for g in range(width // GROUP_CH):
        cols = slice(g * GROUP_CH, (g + 1) * GROUP_CH)
        weight = own_mix_ref[g].astype(jnp.float32)
        masked = jnp.where(keep, weight, 0.0).astype(jnp.bfloat16)
        spatial_ref[:, cols] = lax.dot_general(
            masked, in_ref[:, cols], (((1,), (0,)), ((), ())), preferred_element_type=jnp.float32
        )
        back_ref[:, cols] = lax.dot_general(
            masked, mgrad_ref[:, cols], (((0,), (0,)), ((), ())), preferred_element_type=jnp.float32
        )


def finish_kernel(
    second_ref, recv_ref, cross_mix_ref, gain_ref,
    spatial_ref, back_ref, normed_ref, std_ref, up_slope_ref, gate_slope_ref,
    both_ref, extra_ref,
):
    rows, width = recv_ref.shape
    groups = width // GROUP_CH
    first = second_ref[0] == 0
    spatial_share = jnp.where(first, 0.0, 1.0)
    back_share = jnp.where(first, 1.0, 0.0)

    def mix(dims):
        for g in range(groups):
            cols = slice(g * GROUP_CH, (g + 1) * GROUP_CH)
            extra_ref[:, cols] = lax.dot_general(
                cross_mix_ref[g], recv_ref[:, cols], (dims, ((), ())),
                preferred_element_type=jnp.float32,
            )

    @pl.when(first)
    def _():
        mix(((0,), (0,)))

    @pl.when(jnp.logical_not(first))
    def _():
        mix(((1,), (0,)))

    def body(at):
        extra = extra_ref[at, :]
        spatial = (spatial_ref[at, :] + extra * spatial_share).astype(jnp.bfloat16)
        back = (back_ref[at, :] + extra * back_share).astype(jnp.bfloat16)
        both_ref[at, :width] = (up_slope_ref[at, :] * spatial.astype(jnp.float32)).astype(
            jnp.bfloat16
        )
        scaled = back.astype(jnp.float32) * gain_ref[...]
        normed = normed_ref[at, :]
        mean = jnp.sum(scaled, axis=-1, keepdims=True) * (1.0 / width)
        along = jnp.sum(scaled * normed, axis=-1, keepdims=True) * (1.0 / width)
        gated_grad = std_ref[at, :1] * (scaled - mean - normed * along)
        both_ref[at, width:] = (gated_grad * gate_slope_ref[at, :]).astype(jnp.bfloat16)

    row_loop(rows, body)


def contract(first_op, second_op, dims):
    return lax.dot_general(
        first_op, second_op, (dims, ((), ())), preferred_element_type=jnp.float32
    )


def on_device(inputs, up_pre, gate_pre, cotangent, norm_gain, up_weight, gate_weight, mix_weight):
    sequences, rows, width = cotangent.shape
    model_width = inputs.shape[2]
    sp_count = lax.axis_size("sp")
    assert sequences == 1 and SPAN == 2 * rows
    f32 = lambda *shape: jax.ShapeDtypeStruct(shape, jnp.float32)
    bf16 = lambda *shape: jax.ShapeDtypeStruct(shape, jnp.bfloat16)
    up_flat = up_pre.reshape(rows, width)
    gate_flat = gate_pre.reshape(rows, width)
    grad_flat = cotangent.reshape(rows, width)
    gain = norm_gain.reshape(1, width)
    half = lax.axis_index("sp") % 2
    second = half.astype(jnp.int32).reshape(1)

    moved_inputs = lax.all_to_all(
        inputs.reshape(rows, model_width), "dp", split_axis=1, concat_axis=0, tiled=True
    )

    send = pl.pallas_call(
        send_kernel,
        out_shape=bf16(rows, width),
        in_specs=[SCALAR] + [WHOLE] * 4,
        out_specs=WHOLE,
        name="send_half",
    )(second, up_flat, gate_flat, grad_flat, gain)
    recv = lax.ppermute(send, "sp", [(i, i ^ 1) for i in range(sp_count)])

    groups = mix_weight.shape[0]
    own_mix = lax.dynamic_slice(
        mix_weight, (0, half * rows, half * rows), (groups, rows, rows)
    )
    cross_mix = mix_weight[:, rows:, :rows]
    local = pl.pallas_call(
        own_kernel,
        out_shape=(
            f32(rows, width), f32(rows, width), f32(rows, width),
            f32(rows, GROUP_CH), f32(rows, width), f32(rows, width),
        ),
        in_specs=[WHOLE] * 5,
        out_specs=(WHOLE,) * 6,
        scratch_shapes=[pltpu.VMEM((rows, width), jnp.bfloat16)] * 2,
        cost_estimate=pl.CostEstimate(
            flops=20_000_000_000, transcendentals=0, bytes_accessed=8 * 1024 * 1024
        ),
        name="own_half",
    )(up_flat, gate_flat, grad_flat, gain, own_mix)
    both = pl.pallas_call(
        finish_kernel,
        out_shape=bf16(rows, 2 * width),
        in_specs=[SCALAR] + [WHOLE] * 9,
        out_specs=WHOLE,
        scratch_shapes=[pltpu.VMEM((rows, width), jnp.float32)],
        name="finish",
    )(second, recv, cross_mix, gain, *local)

    every = lax.all_gather(both, "dp", axis=0, tiled=True)
    part = contract(moved_inputs, every, ((0,), (0,))).astype(jnp.bfloat16)
    own_part = lax.psum_scatter(part, "sp", scatter_dimension=0, tiled=True)
    weight_rows = lax.all_gather(own_part, "sp", axis=0, tiled=True)

    columns = (
        contract(every[:, :width], up_weight, ((1,), (1,)))
        + contract(every[:, width:], gate_weight, ((1,), (1,)))
    ).astype(jnp.bfloat16)
    input_grad = lax.all_to_all(columns, "dp", split_axis=0, concat_axis=1, tiled=True)
    input_grad = input_grad.reshape(sequences, rows, model_width)
    up_weight_grad = weight_rows[:, :width].astype(jnp.float32) * grad_scale
    gate_weight_grad = weight_rows[:, width:].astype(jnp.float32) * grad_scale
    return (input_grad, up_weight_grad, gate_weight_grad)


def solution(mesh):
    return jax.shard_map(
        on_device,
        mesh=mesh,
        in_specs=(
            P("dp", "sp", None),
            P("dp", "sp", None),
            P("dp", "sp", None),
            P("dp", "sp", None),
            P(),
            P("dp", None),
            P("dp", None),
            P(),
        ),
        out_specs=(P("dp", "sp", None), P("dp", None), P("dp", None)),
        check_vma=False,
    )
```

```python
import math

import jax
import jax.numpy as jnp
from jax import lax
from jax.experimental import pallas as pl
from jax.experimental.pallas import tpu as pltpu
from jax.sharding import PartitionSpec as P

GROUP_CH = 128
SPAN = 512
SEG = 64
ROW_STEP = 32

norm_eps = 1e-05
grad_scale = 1.0 / 256.0
root_half = 1.0 / math.sqrt(2.0)
root_twopi = 1.0 / math.sqrt(2.0 * math.pi)

WHOLE = pl.BlockSpec(memory_space=pltpu.VMEM)
SCALAR = pl.BlockSpec(memory_space=pltpu.SMEM)


def normal_cdf(preact):
    return 0.5 * (1.0 + lax.erf(preact * root_half))


def gelu_slope(preact, cdf):
    return cdf + preact * jnp.exp(-0.5 * preact * preact) * root_twopi


def norm_stats(gate):
    gated_act = gate * normal_cdf(gate)
    width = gate.shape[1]
    centered = gated_act - jnp.sum(gated_act, axis=-1, keepdims=True) * (1.0 / width)
    variance = jnp.sum(centered * centered, axis=-1, keepdims=True) * (1.0 / width)
    inverse_std = lax.rsqrt(variance + norm_eps)
    return centered * inverse_std, inverse_std


def row_loop(rows, body):
    def step(at, carry):
        body(pl.ds(pl.multiple_of(at * ROW_STEP, ROW_STEP), ROW_STEP))
        return carry

    lax.fori_loop(0, rows // ROW_STEP, step, 0)


def send_kernel(second_ref, up_ref, gate_ref, grad_ref, gain_ref, send_ref):
    rows = up_ref.shape[0]

    @pl.when(second_ref[0] == 0)
    def _():
        def body(at):
            normed, _ = norm_stats(gate_ref[at, :].astype(jnp.float32))
            send_ref[at, :] = (normed * gain_ref[...]).astype(jnp.bfloat16)

        row_loop(rows, body)

    @pl.when(second_ref[0] != 0)
    def _():
        def body(at):
            up = up_ref[at, :].astype(jnp.float32)
            mixed = grad_ref[at, :].astype(jnp.float32) * (up * normal_cdf(up))
            send_ref[at, :] = mixed.astype(jnp.bfloat16)

        row_loop(rows, body)


def own_kernel(
    up_ref, gate_ref, grad_ref, gain_ref, own_mix_ref,
    spatial_ref, back_ref, normed_ref, std_ref, up_slope_ref, gate_slope_ref,
    in_ref, mgrad_ref,
):
    rows, width = up_ref.shape

    def body(at):
        gate = gate_ref[at, :].astype(jnp.float32)
        normed, inverse_std = norm_stats(gate)
        normed_ref[at, :] = normed
        std_ref[at, :] = jnp.broadcast_to(inverse_std, (ROW_STEP, GROUP_CH))
        in_ref[at, :] = (normed * gain_ref[...]).astype(jnp.bfloat16)
        gate_slope_ref[at, :] = gelu_slope(gate, normal_cdf(gate))
        up = up_ref[at, :].astype(jnp.float32)
        grad = grad_ref[at, :].astype(jnp.float32)
        cdf = normal_cdf(up)
        mgrad_ref[at, :] = (grad * (up * cdf)).astype(jnp.bfloat16)
        up_slope_ref[at, :] = grad * gelu_slope(up, cdf)

    row_loop(rows, body)
    row_seg = lax.broadcasted_iota(jnp.int32, (rows, rows), 0) // SEG
    col_seg = lax.broadcasted_iota(jnp.int32, (rows, rows), 1) // SEG
    keep = col_seg <= row_seg
    for g in range(width // GROUP_CH):
        cols = slice(g * GROUP_CH, (g + 1) * GROUP_CH)
        weight = own_mix_ref[g].astype(jnp.float32)
        masked = jnp.where(keep, weight, 0.0).astype(jnp.bfloat16)
        spatial_ref[:, cols] = lax.dot_general(
            masked, in_ref[:, cols], (((1,), (0,)), ((), ())), preferred_element_type=jnp.float32
        )
        back_ref[:, cols] = lax.dot_general(
            masked, mgrad_ref[:, cols], (((0,), (0,)), ((), ())), preferred_element_type=jnp.float32
        )


def finish_kernel(
    second_ref, recv_ref, cross_mix_ref, gain_ref,
    spatial_ref, back_ref, normed_ref, std_ref, up_slope_ref, gate_slope_ref,
    up_out_ref, gate_out_ref, extra_ref,
):
    rows, width = recv_ref.shape
    groups = width // GROUP_CH
    first = second_ref[0] == 0
    spatial_share = jnp.where(first, 0.0, 1.0)
    back_share = jnp.where(first, 1.0, 0.0)

    def mix(dims):
        for g in range(groups):
            cols = slice(g * GROUP_CH, (g + 1) * GROUP_CH)
            extra_ref[:, cols] = lax.dot_general(
                cross_mix_ref[g], recv_ref[:, cols], (dims, ((), ())),
                preferred_element_type=jnp.float32,
            )

    @pl.when(first)
    def _():
        mix(((0,), (0,)))

    @pl.when(jnp.logical_not(first))
    def _():
        mix(((1,), (0,)))

    def body(at):
        extra = extra_ref[at, :]
        spatial = (spatial_ref[at, :] + extra * spatial_share).astype(jnp.bfloat16)
        back = (back_ref[at, :] + extra * back_share).astype(jnp.bfloat16)
        up_out_ref[at, :] = (up_slope_ref[at, :] * spatial.astype(jnp.float32)).astype(
            jnp.bfloat16
        )
        scaled = back.astype(jnp.float32) * gain_ref[...]
        normed = normed_ref[at, :]
        mean = jnp.sum(scaled, axis=-1, keepdims=True) * (1.0 / width)
        along = jnp.sum(scaled * normed, axis=-1, keepdims=True) * (1.0 / width)
        gated_grad = std_ref[at, :1] * (scaled - mean - normed * along)
        gate_out_ref[at, :] = (gated_grad * gate_slope_ref[at, :]).astype(jnp.bfloat16)

    row_loop(rows, body)


def contract(first_op, second_op, dims):
    return lax.dot_general(
        first_op, second_op, (dims, ((), ())), preferred_element_type=jnp.float32
    )


def exchange(value, axis, flip):
    count = lax.axis_size(axis)
    return lax.ppermute(value, axis, [(i, i ^ flip) for i in range(count)])


def unscramble(blocks, digit, axis):
    bit = 1
    while bit < len(blocks):
        odd = (digit & bit) != 0
        blocks = [jnp.where(odd, blocks[b ^ bit], blocks[b]) for b in range(len(blocks))]
        bit *= 2
    return jnp.concatenate(blocks, axis=axis)


def sum_stages(count):
    stages = [(0, 2)]
    offset = 1
    while (1 << offset) < count:
        radix = min(4, count >> offset)
        stages.append((offset, radix))
        offset += radix.bit_length() - 1
    return stages


def sum_over_sp(part, stages):
    index = lax.axis_index("sp")
    for offset, radix in stages:
        digit = (index >> offset) & (radix - 1)
        size = part.shape[0] // radix
        arrived = [
            exchange(
                lax.dynamic_slice_in_dim(part, (digit ^ r) * size, size, 0).astype(jnp.bfloat16),
                "sp",
                r << offset,
            )
            for r in range(1, radix)
        ]
        part = lax.dynamic_slice_in_dim(part, digit * size, size, 0)
        for piece in arrived:
            part = part + piece.astype(jnp.float32)
    rows = part.astype(jnp.bfloat16)
    for offset, radix in reversed(stages):
        digit = (index >> offset) & (radix - 1)
        blocks = [rows] + [exchange(rows, "sp", r << offset) for r in range(1, radix)]
        rows = unscramble(blocks, digit, 0)
    return rows


def on_device(inputs, up_pre, gate_pre, cotangent, norm_gain, up_weight, gate_weight, mix_weight):
    sequences, rows, width = cotangent.shape
    model_width = inputs.shape[2]
    sp_count = lax.axis_size("sp")
    assert sequences == 1 and SPAN == 2 * rows
    f32 = lambda *shape: jax.ShapeDtypeStruct(shape, jnp.float32)
    bf16 = lambda *shape: jax.ShapeDtypeStruct(shape, jnp.bfloat16)
    up_flat = up_pre.reshape(rows, width)
    gate_flat = gate_pre.reshape(rows, width)
    grad_flat = cotangent.reshape(rows, width)
    gain = norm_gain.reshape(1, width)
    half = lax.axis_index("sp") % 2
    second = half.astype(jnp.int32).reshape(1)

    send = pl.pallas_call(
        send_kernel,
        out_shape=bf16(rows, width),
        in_specs=[SCALAR] + [WHOLE] * 4,
        out_specs=WHOLE,
        name="send_half",
    )(second, up_flat, gate_flat, grad_flat, gain)
    recv = exchange(send, "sp", 1)

    dp_count = lax.axis_size("dp")
    dp_index = lax.axis_index("dp")
    share = model_width // dp_count
    flat_inputs = inputs.reshape(rows, model_width)
    moved = [
        lax.dynamic_slice_in_dim(flat_inputs, (dp_index ^ r) * share, share, 1)
        for r in range(dp_count)
    ]
    moved = moved[:1] + [exchange(moved[r], "dp", r) for r in range(1, dp_count)]

    groups = mix_weight.shape[0]
    own_mix = lax.dynamic_slice(
        mix_weight, (0, half * rows, half * rows), (groups, rows, rows)
    )
    cross_mix = mix_weight[:, rows:, :rows]
    local = pl.pallas_call(
        own_kernel,
        out_shape=(
            f32(rows, width), f32(rows, width), f32(rows, width),
            f32(rows, GROUP_CH), f32(rows, width), f32(rows, width),
        ),
        in_specs=[WHOLE] * 5,
        out_specs=(WHOLE,) * 6,
        scratch_shapes=[pltpu.VMEM((rows, width), jnp.bfloat16)] * 2,
        cost_estimate=pl.CostEstimate(
            flops=20_000_000_000, transcendentals=0, bytes_accessed=8 * 1024 * 1024
        ),
        name="own_half",
    )(up_flat, gate_flat, grad_flat, gain, own_mix)
    up_grad, gate_grad = pl.pallas_call(
        finish_kernel,
        out_shape=(bf16(rows, width), bf16(rows, width)),
        in_specs=[SCALAR] + [WHOLE] * 9,
        out_specs=(WHOLE, WHOLE),
        scratch_shapes=[pltpu.VMEM((rows, width), jnp.float32)],
        name="finish",
    )(second, recv, cross_mix, gain, *local)

    stages = sum_stages(sp_count)
    up_all = [up_grad] + [exchange(up_grad, "dp", r) for r in range(1, dp_count)]
    gate_all = [gate_grad] + [exchange(gate_grad, "dp", r) for r in range(1, dp_count)]
    up_part = sum(contract(moved[r], up_all[r], ((0,), (0,))) for r in range(dp_count))
    up_rows = sum_over_sp(up_part, stages)
    gate_part = sum(contract(moved[r], gate_all[r], ((0,), (0,))) for r in range(dp_count))
    gate_rows = sum_over_sp(gate_part, stages[1:] + stages[:1])
    columns = [
        (
            contract(up_all[r], up_weight, ((1,), (1,)))
            + contract(gate_all[r], gate_weight, ((1,), (1,)))
        ).astype(jnp.bfloat16)
        for r in range(dp_count)
    ]
    columns = columns[:1] + [exchange(columns[r], "dp", r) for r in range(1, dp_count)]
    input_grad = unscramble(columns, dp_index, 1).reshape(sequences, rows, model_width)
    up_weight_grad = up_rows.astype(jnp.float32) * grad_scale
    gate_weight_grad = gate_rows.astype(jnp.float32) * grad_scale
    return (input_grad, up_weight_grad, gate_weight_grad)


def solution(mesh):
    return jax.shard_map(
        on_device,
        mesh=mesh,
        in_specs=(
            P("dp", "sp", None),
            P("dp", "sp", None),
            P("dp", "sp", None),
            P("dp", "sp", None),
            P(),
            P("dp", None),
            P("dp", None),
            P(),
        ),
        out_specs=(P("dp", "sp", None), P("dp", None), P("dp", None)),
        check_vma=False,
    )
```

```python
import math

import jax
import jax.numpy as jnp
from jax import lax
from jax.experimental import pallas as pl
from jax.experimental.pallas import tpu as pltpu
from jax.sharding import PartitionSpec as P

GROUP_CH = 128
SPAN = 512
SEG = 64
ROW_STEP = 32

norm_eps = 1e-05
grad_scale = 1.0 / 256.0
root_half = 1.0 / math.sqrt(2.0)
root_twopi = 1.0 / math.sqrt(2.0 * math.pi)

WHOLE = pl.BlockSpec(memory_space=pltpu.VMEM)
SCALAR = pl.BlockSpec(memory_space=pltpu.SMEM)


def normal_cdf(preact):
    return 0.5 * (1.0 + lax.erf(preact * root_half))


def gelu_slope(preact, cdf):
    return cdf + preact * jnp.exp(-0.5 * preact * preact) * root_twopi


def norm_stats(gate):
    gated_act = gate * normal_cdf(gate)
    width = gate.shape[1]
    centered = gated_act - jnp.sum(gated_act, axis=-1, keepdims=True) * (1.0 / width)
    variance = jnp.sum(centered * centered, axis=-1, keepdims=True) * (1.0 / width)
    inverse_std = lax.rsqrt(variance + norm_eps)
    return centered * inverse_std, inverse_std


def row_loop(rows, body):
    def step(at, carry):
        body(pl.ds(pl.multiple_of(at * ROW_STEP, ROW_STEP), ROW_STEP))
        return carry

    lax.fori_loop(0, rows // ROW_STEP, step, 0)


def send_kernel(second_ref, up_ref, gate_ref, grad_ref, gain_ref, send_ref):
    rows = up_ref.shape[0]

    @pl.when(second_ref[0] == 0)
    def _():
        def body(at):
            normed, _ = norm_stats(gate_ref[at, :].astype(jnp.float32))
            send_ref[at, :] = (normed * gain_ref[...]).astype(jnp.bfloat16)

        row_loop(rows, body)

    @pl.when(second_ref[0] != 0)
    def _():
        def body(at):
            up = up_ref[at, :].astype(jnp.float32)
            mixed = grad_ref[at, :].astype(jnp.float32) * (up * normal_cdf(up))
            send_ref[at, :] = mixed.astype(jnp.bfloat16)

        row_loop(rows, body)


def own_kernel(
    up_ref, gate_ref, grad_ref, gain_ref, own_mix_ref,
    spatial_ref, back_ref, normed_ref, std_ref, up_slope_ref, gate_slope_ref,
    in_ref, mgrad_ref,
):
    rows, width = up_ref.shape

    def body(at):
        gate = gate_ref[at, :].astype(jnp.float32)
        normed, inverse_std = norm_stats(gate)
        normed_ref[at, :] = normed
        std_ref[at, :] = jnp.broadcast_to(inverse_std, (ROW_STEP, GROUP_CH))
        in_ref[at, :] = (normed * gain_ref[...]).astype(jnp.bfloat16)
        gate_slope_ref[at, :] = gelu_slope(gate, normal_cdf(gate))
        up = up_ref[at, :].astype(jnp.float32)
        grad = grad_ref[at, :].astype(jnp.float32)
        cdf = normal_cdf(up)
        mgrad_ref[at, :] = (grad * (up * cdf)).astype(jnp.bfloat16)
        up_slope_ref[at, :] = grad * gelu_slope(up, cdf)

    row_loop(rows, body)
    row_seg = lax.broadcasted_iota(jnp.int32, (rows, rows), 0) // SEG
    col_seg = lax.broadcasted_iota(jnp.int32, (rows, rows), 1) // SEG
    keep = col_seg <= row_seg
    for g in range(width // GROUP_CH):
        cols = slice(g * GROUP_CH, (g + 1) * GROUP_CH)
        weight = own_mix_ref[g].astype(jnp.float32)
        masked = jnp.where(keep, weight, 0.0).astype(jnp.bfloat16)
        spatial_ref[:, cols] = lax.dot_general(
            masked, in_ref[:, cols], (((1,), (0,)), ((), ())), preferred_element_type=jnp.float32
        )
        back_ref[:, cols] = lax.dot_general(
            masked, mgrad_ref[:, cols], (((0,), (0,)), ((), ())), preferred_element_type=jnp.float32
        )


def cross_terms(second_ref, recv_ref, cross_mix_ref, base_ref, total_ref, wanted, dims):
    width = recv_ref.shape[1]

    @pl.when(second_ref[0] == wanted)
    def _():
        for g in range(width // GROUP_CH):
            cols = slice(g * GROUP_CH, (g + 1) * GROUP_CH)
            extra = lax.dot_general(
                cross_mix_ref[g], recv_ref[:, cols], (dims, ((), ())),
                preferred_element_type=jnp.float32,
            )
            total_ref[:, cols] = (base_ref[:, cols] + extra).astype(jnp.bfloat16)

    @pl.when(second_ref[0] != wanted)
    def _():
        total_ref[...] = base_ref[...].astype(jnp.bfloat16)


def finish_up_kernel(
    second_ref, recv_ref, cross_mix_ref, spatial_ref, up_slope_ref, out_ref, total_ref
):
    cross_terms(
        second_ref, recv_ref, cross_mix_ref, spatial_ref, total_ref, 1, ((1,), (0,))
    )

    def body(at):
        spatial = total_ref[at, :].astype(jnp.float32)
        out_ref[at, :] = (up_slope_ref[at, :] * spatial).astype(jnp.bfloat16)

    row_loop(recv_ref.shape[0], body)


def finish_gate_kernel(
    second_ref, recv_ref, cross_mix_ref, gain_ref, back_ref, normed_ref, std_ref,
    gate_slope_ref, earlier_ref, out_ref, total_ref,
):
    width = recv_ref.shape[1]
    cross_terms(second_ref, recv_ref, cross_mix_ref, back_ref, total_ref, 0, ((0,), (0,)))

    def body(at):
        scaled = total_ref[at, :].astype(jnp.float32) * gain_ref[...]
        normed = normed_ref[at, :]
        mean = jnp.sum(scaled, axis=-1, keepdims=True) * (1.0 / width)
        along = jnp.sum(scaled * normed, axis=-1, keepdims=True) * (1.0 / width)
        gated_grad = std_ref[at, :1] * (scaled - mean - normed * along)
        out_ref[at, :] = (gated_grad * gate_slope_ref[at, :]).astype(jnp.bfloat16)

    row_loop(recv_ref.shape[0], body)


def over_dp(value, dp_count, mark=None):
    values = [value] + [exchange(value, "dp", r) for r in range(2, dp_count, 2)]
    if mark is not None:
        values = values[:1] + [after(near, mark) for near in values[1:]]
    pairs = [(near, exchange(near, "dp", 1)) for near in values]
    return [value for pair in pairs for value in pair]


def contract(first_op, second_op, dims):
    return lax.dot_general(
        first_op, second_op, (dims, ((), ())), preferred_element_type=jnp.float32
    )


def exchange(value, axis, flip):
    count = lax.axis_size(axis)
    return lax.ppermute(value, axis, [(i, i ^ flip) for i in range(count)])


def after(value, mark):
    return lax.optimization_barrier((value, mark))[0]


def unscramble(blocks, digit, axis):
    bit = 1
    while bit < len(blocks):
        odd = (digit & bit) != 0
        blocks = [jnp.where(odd, blocks[b ^ bit], blocks[b]) for b in range(len(blocks))]
        bit *= 2
    return jnp.concatenate(blocks, axis=axis)


def sum_stages(count):
    stages = [(0, 2)]
    offset = 1
    while (1 << offset) < count:
        radix = min(4, count >> offset)
        stages.append((offset, radix))
        offset += radix.bit_length() - 1
    return stages


def sum_over_sp(part, stages, marks):
    index = lax.axis_index("sp")
    for offset, radix in stages:
        digit = (index >> offset) & (radix - 1)
        size = part.shape[0] // radix
        pieces = [
            lax.dynamic_slice_in_dim(part, (digit ^ r) * size, size, 0).astype(jnp.bfloat16)
            for r in range(1, radix)
        ]
        marks.append(pieces[-1])
        arrived = [exchange(pieces[r - 1], "sp", r << offset) for r in range(1, radix)]
        part = lax.dynamic_slice_in_dim(part, digit * size, size, 0)
        for piece in arrived:
            part = part + piece.astype(jnp.float32)
    rows = part.astype(jnp.bfloat16)
    marks.append(rows)
    for offset, radix in reversed(stages):
        digit = (index >> offset) & (radix - 1)
        blocks = [rows] + [exchange(rows, "sp", r << offset) for r in range(1, radix)]
        rows = unscramble(blocks, digit, 0)
    return rows


def on_device(inputs, up_pre, gate_pre, cotangent, norm_gain, up_weight, gate_weight, mix_weight):
    sequences, rows, width = cotangent.shape
    model_width = inputs.shape[2]
    sp_count = lax.axis_size("sp")
    assert sequences == 1 and SPAN == 2 * rows
    f32 = lambda *shape: jax.ShapeDtypeStruct(shape, jnp.float32)
    bf16 = lambda *shape: jax.ShapeDtypeStruct(shape, jnp.bfloat16)
    up_flat = up_pre.reshape(rows, width)
    gate_flat = gate_pre.reshape(rows, width)
    grad_flat = cotangent.reshape(rows, width)
    gain = norm_gain.reshape(1, width)
    half = lax.axis_index("sp") % 2
    second = half.astype(jnp.int32).reshape(1)

    send = pl.pallas_call(
        send_kernel,
        out_shape=bf16(rows, width),
        in_specs=[SCALAR] + [WHOLE] * 4,
        out_specs=WHOLE,
        name="send_half",
    )(second, up_flat, gate_flat, grad_flat, gain)
    recv = exchange(send, "sp", 1)

    dp_count = lax.axis_size("dp")
    dp_index = lax.axis_index("dp")
    share = model_width // dp_count
    flat_inputs = inputs.reshape(rows, model_width)
    moved = [
        lax.dynamic_slice_in_dim(flat_inputs, (dp_index ^ r) * share, share, 1)
        for r in range(dp_count)
    ]
    moved = moved[:1] + [exchange(moved[r], "dp", r) for r in range(1, dp_count)]

    groups = mix_weight.shape[0]
    own_mix = lax.dynamic_slice(
        mix_weight, (0, half * rows, half * rows), (groups, rows, rows)
    )
    cross_mix = mix_weight[:, rows:, :rows]
    spatial, back, normed, inverse_std, up_slope, gate_slope = pl.pallas_call(
        own_kernel,
        out_shape=(
            f32(rows, width), f32(rows, width), f32(rows, width),
            f32(rows, GROUP_CH), f32(rows, width), f32(rows, width),
        ),
        in_specs=[WHOLE] * 5,
        out_specs=(WHOLE,) * 6,
        scratch_shapes=[pltpu.VMEM((rows, width), jnp.bfloat16)] * 2,
        cost_estimate=pl.CostEstimate(
            flops=20_000_000_000, transcendentals=0, bytes_accessed=8 * 1024 * 1024
        ),
        name="own_half",
    )(up_flat, gate_flat, grad_flat, gain, own_mix)
    total = [pltpu.VMEM((rows, width), jnp.bfloat16)]
    up_grad = pl.pallas_call(
        finish_up_kernel,
        out_shape=bf16(rows, width),
        in_specs=[SCALAR] + [WHOLE] * 4,
        out_specs=WHOLE,
        scratch_shapes=total,
        name="finish_up",
    )(second, recv, cross_mix, spatial, up_slope)
    up_all = over_dp(up_grad, dp_count)
    gate_grad = pl.pallas_call(
        finish_gate_kernel,
        out_shape=bf16(rows, width),
        in_specs=[SCALAR] + [WHOLE] * 7 + [pl.BlockSpec(memory_space=pl.ANY)],
        out_specs=WHOLE,
        scratch_shapes=total,
        name="finish_gate",
    )(second, recv, cross_mix, gain, back, normed, inverse_std, gate_slope, up_grad)
    stages = sum_stages(sp_count)
    up_marks, gate_marks = [], []
    up_part = sum(contract(moved[r], up_all[r], ((0,), (0,))) for r in range(dp_count))
    up_rows = sum_over_sp(up_part, stages, up_marks)
    gate_all = over_dp(gate_grad, dp_count, up_marks[0])
    gate_part = sum(contract(moved[r], gate_all[r], ((0,), (0,))) for r in range(dp_count))
    gate_rows = sum_over_sp(gate_part, stages, gate_marks)
    up_late = after(up_weight, up_marks[1])
    gate_late = after(gate_weight, gate_marks[0])
    columns = [
        (
            contract(up_all[r], up_late, ((1,), (1,)))
            + contract(gate_all[r], gate_late, ((1,), (1,)))
        ).astype(jnp.bfloat16)
        for r in range(dp_count)
    ]
    columns = columns[:1] + [
        after(exchange(columns[r], "dp", r), up_marks[-1]) for r in range(1, dp_count)
    ]
    input_grad = unscramble(columns, dp_index, 1).reshape(sequences, rows, model_width)
    up_weight_grad = up_rows.astype(jnp.float32) * grad_scale
    gate_weight_grad = gate_rows.astype(jnp.float32) * grad_scale
    return (input_grad, up_weight_grad, gate_weight_grad)


def solution(mesh):
    return jax.shard_map(
        on_device,
        mesh=mesh,
        in_specs=(
            P("dp", "sp", None),
            P("dp", "sp", None),
            P("dp", "sp", None),
            P("dp", "sp", None),
            P(),
            P("dp", None),
            P("dp", None),
            P(),
        ),
        out_specs=(P("dp", "sp", None), P("dp", None), P("dp", None)),
        check_vma=False,
    )
```
